32 devices in a mesh: kv: 8 (over z, y), tp: 4 (over x, core).
Axes of the slice: x: 2, y: 2, z: 4, core: 2. Of those that a mesh axis runs over, the one named last changes fastest.
Arguments:
- tokens: bfloat16 [16, 4096], P(None, ('kv', 'tp')), may hold values from -6 to 6
- gain_attn: bfloat16 [4096], replicated, may hold values from 0.099609375 to 1.8984375
- w_query: bfloat16 [4096, 2048], P('kv', 'tp'), may hold values from -0.09375 to 0.09375
- w_key: bfloat16 [4096, 2048], P('kv', 'tp'), may hold values from -0.09375 to 0.09375
- w_value: bfloat16 [4096, 2048], P('kv', 'tp'), may hold values from -0.09375 to 0.09375
- w_forget: bfloat16 [4096, 32], replicated, may hold values from -0.09375 to 0.09375
- forget_bias: float32 [32], replicated, may hold values from -2 to 2
- keys_cache: bfloat16 [16, 4096, 2048], P(None, 'kv', 'tp'), may hold values from -900 to 900
- values_cache: bfloat16 [16, 4096, 2048], P(None, 'kv', 'tp'), may hold values from -6 to 6
- gates_cache: float32 [16, 32, 4096], P(None, 'tp', 'kv'), as said below
- lengths: int32 [16], replicated, may hold values from 1 to 4096, 32768 in all
- w_out: bfloat16 [2048, 4096], P('tp', 'kv'), may hold values from -0.1875 to 0.1875
- gain_mixer: bfloat16 [4096], replicated, may hold values from 0.099609375 to 1.8984375
- w_up: bfloat16 [4096, 16384], P('kv', 'tp'), may hold values from -0.09375 to 0.09375
- w_down: bfloat16 [16384, 4096], P('tp', 'kv'), may hold values from -0.0625 to 0.0625
Outputs:
- output: bfloat16 [16, 4096], P(None, ('kv', 'tp'))
The draws below stay inside these ranges and needn't reach their ends.
Inputs may be any that keep to these rules, and one draw needn't show every extreme that they name: One sequence has all 4096 positions live; the lengths add up to half of 16 times 4096. `gates_cache`: along positions each entry is the running sum of per-position log forget gates up to and including that position, so the values never rise.
All inputs are finite; a program needn't handle non-finite values.
Results may differ from the reference program's by a relative error of at most 0.017.
Values may be sent and summed in bfloat16 or wider, within the bound.
No kernel may reach another device: no remote copies, remote signals or barrier semaphores. Data moves between devices by JAX's collectives and lax.ppermute only.
A program may use at most 128 MiB of HBM per device.

```python
import math
import jax
import jax.numpy as jnp
import numpy as np
from jax import lax

D = 4096
ATTENDER_NUMBER = 32
FF = 16384
BATCH_STRINGS = 16
STORED_POSITIONS = 4096
QW = 2048
N_KV = 8
N_TP = 4


def draw_gates_cache(key, part):
    split_prng_material = jax.random.split(jax.random.fold_in(key, 7), 6)
    share = 0.5
    slow_heads = jax.random.uniform(split_prng_material[0], (ATTENDER_NUMBER,)) < share
    slow_rate = jnp.exp(jax.random.uniform(split_prng_material[1], (ATTENDER_NUMBER,), minval=jnp.log(0.2), maxval=jnp.log(0.8))) / STORED_POSITIONS
    fast_rate = jnp.exp(jax.random.uniform(split_prng_material[2], (ATTENDER_NUMBER,), minval=jnp.log(0.01), maxval=jnp.log(1.0 / 30.0)))
    rate = jnp.where(slow_heads, slow_rate, fast_rate)
    factor = jnp.exp(jax.random.uniform(split_prng_material[3], (BATCH_STRINGS, ATTENDER_NUMBER, N_KV), minval=-0.7, maxval=0.7))
    factor = jnp.repeat(factor, STORED_POSITIONS // N_KV, axis=-1)
    rough = jax.random.uniform(split_prng_material[4], (BATCH_STRINGS, ATTENDER_NUMBER, STORED_POSITIONS), minval=0.5, maxval=1.5)
    decoding_logarithmic_decays = -rate[None, :, None] * factor * rough
    draw_filled_extents = jax.random.uniform(split_prng_material[5], (2, BATCH_STRINGS, ATTENDER_NUMBER, STORED_POSITIONS))
    filled_extents = jnp.where(draw_filled_extents[0] < 3.0 / STORED_POSITIONS, jnp.log(0.5 + 0.3 * draw_filled_extents[1]), 0.0)
    return jnp.cumsum(decoding_logarithmic_decays + filled_extents, axis=-1).astype(jnp.float32)


def draw_keys_cache(key, part):
    split_prng_material = jax.random.split(jax.random.fold_in(key, 11), 1)
    base = jnp.clip(jax.random.normal(split_prng_material[0], (BATCH_STRINGS, STORED_POSITIONS, QW), jnp.float32), -6.0, 6.0)
    return base.astype(jnp.bfloat16)


def with_spikes(array, key, source, target, parts, factor):
    owner, partner = [(jnp.arange(array.shape[dim]) // (array.shape[dim] // parts)).reshape([-1 if axis == dim else 1 for axis in range(array.ndim)]) for dim in (source, target)]
    chosen = jax.random.permutation(key, parts)[partner]
    strong = (owner == chosen) | (owner == (partner + parts // 2) % parts)
    return jnp.where(strong, factor * array, array)


def level_of(rng, shape, pieces, least, top_value):
    level, own = 1.0, jax.random.fold_in(rng, 6)
    for position, parts in pieces:
        draws = jnp.exp(jax.random.uniform(jax.random.fold_in(own, position), (parts,), jnp.float32, least / len(pieces), top_value / len(pieces)))
        level = level * jnp.repeat(draws, shape[position] // parts).reshape([-1 if axis == position else 1 for axis in range(len(shape))])
    return level


def profile(number_of, total, most, slope):
    weights = [(1 << 20) // math.isqrt(grade ** slope) + 1 for grade in range(2, number_of + 1)]
    rest, counts = total - most - (number_of - 1), [1] * (number_of - 1)
    while rest > 0:
        candidates = [i for i in range(number_of - 1) if counts[i] < most]
        mass, left = sum([weights[i] for i in candidates]), rest
        for i in candidates:
            more = min(most - counts[i], max(1, left * weights[i] // mass), rest)
            counts[i] = counts[i] + more
            rest = rest - more
    return np.array([most] + counts)


def ragged_sizes(stream_key, number_of, total, bound, lean):
    if number_of == 2:
        one = jax.random.randint(stream_key, (), max(1, total - bound), min(bound, total - 1) + 1)
        return jnp.stack([one, total - one])
    sizes = jnp.asarray(profile(number_of, total, bound, lean), jnp.int32)
    couples = (number_of - 1) // 2
    giver, sink = sizes[1:1 + 2 * couples:2], sizes[2:2 + 2 * couples:2]
    slack = jnp.minimum(giver - 1, bound - sink)
    moved = jax.random.randint(jax.random.fold_in(stream_key, 1), (couples,), 0, 1 << 20) % (slack + 1)
    sizes = sizes.at[1:1 + 2 * couples:2].set(giver - moved).at[2:2 + 2 * couples:2].set(sink + moved)
    return sizes[jax.random.permutation(jax.random.fold_in(stream_key, 2), number_of)]


def normal_values(own_key, shape, width, most, shards=(), kind=jnp.bfloat16):
    result = width * jax.random.normal(own_key, shape, jnp.float32)
    if shards:
        result = result * level_of(own_key, shape, shards, -0.22, 0.18)
    return jnp.clip(result, -most, most).astype(kind)


def heavy_noise(rng, extent, width, reach, cuts, heavy, kind=jnp.bfloat16):
    drawn = width * jax.random.normal(rng, extent, jnp.float32)
    if cuts:
        drawn = drawn * level_of(rng, extent, cuts, -0.22, 0.18)
    return jnp.clip(with_spikes(drawn, jax.random.fold_in(rng, 3), *heavy), -reach, reach).astype(kind)


def setup_inputs(seed: int = 0) -> dict:
    streams_of = jax.random.split(jax.random.key(seed), 16)
    return {
        "tokens": normal_values(streams_of[0], (BATCH_STRINGS, D), 1.0, 6.0, ((1, 32),)),
        "gain_attn": jnp.clip(1.0 + 0.18 * jax.random.normal(streams_of[1], (D,), jnp.float32), 0.099609375, 1.8984375).astype(jnp.bfloat16),
        "w_query": normal_values(streams_of[2], (D, QW), D ** -0.5, 0.09375, ((0, 8), (1, 4))),
        "w_key": normal_values(streams_of[3], (D, QW), D ** -0.5, 0.09375, ((0, 8), (1, 4))),
        "w_value": normal_values(streams_of[4], (D, QW), D ** -0.5, 0.09375, ((0, 8), (1, 4))),
        "w_forget": normal_values(streams_of[5], (D, ATTENDER_NUMBER), D ** -0.5, 0.09375),
        "forget_bias": jnp.clip(jax.random.uniform(streams_of[6], (ATTENDER_NUMBER,), jnp.float32, -2.0, 2.0), -2.0, 2.0),
        "keys_cache": draw_keys_cache(jax.random.fold_in(streams_of[15], 71), 0),
        "values_cache": normal_values(streams_of[8], (BATCH_STRINGS, STORED_POSITIONS, QW), 1.0, 6.0, ((1, 8), (2, 4))),
        "gates_cache": draw_gates_cache(jax.random.fold_in(streams_of[15], 71), 0),
        "lengths": ragged_sizes(streams_of[10], BATCH_STRINGS, BATCH_STRINGS * STORED_POSITIONS // 2, STORED_POSITIONS, 2).astype(jnp.int32),
        "w_out": heavy_noise(streams_of[11], (QW, D), QW ** -0.5, 0.1875, ((0, 4), (1, 8)), (0, 1, 8, 2.0)),
        "gain_mixer": jnp.clip(1.0 + 0.18 * jax.random.normal(streams_of[12], (D,), jnp.float32), 0.099609375, 1.8984375).astype(jnp.bfloat16),
        "w_up": normal_values(streams_of[13], (D, FF), D ** -0.5, 0.09375, ((0, 8), (1, 4))),
        "w_down": heavy_noise(streams_of[14], (FF, D), FF ** -0.5, 0.0625, ((0, 4), (1, 8)), (0, 1, 8, 2.0)),
    }


norm_eps = 1e-06

def attend_one(items):
    query, keys, values, gates, length, forget_log, new_key, new_value = items
    heads = gates.shape[0]
    query_f = query.reshape(heads, -1).astype(jnp.float32)
    scale = query_f.shape[-1] ** (-0.5)
    keys_f = keys.reshape(keys.shape[0], heads, -1).astype(jnp.float32)
    values_f = values.reshape(values.shape[0], heads, -1).astype(jnp.float32)
    scores = jnp.einsum('hd,lhd->hl', query_f, keys_f) * scale
    last_gate = lax.dynamic_slice_in_dim(gates, (length - 1).astype(jnp.int32), 1, 1)[:, 0]
    logits = scores + (last_gate + forget_log)[:, None] - gates
    valid = jnp.arange(gates.shape[1], dtype=jnp.int32) < length
    logits = jnp.where(valid[None, :], logits, -jnp.inf)
    own = lax.optimization_barrier(jnp.sum(query_f * new_key.reshape(heads, -1).astype(jnp.float32), axis=-1)) * scale
    top = jnp.maximum(lax.optimization_barrier(jnp.max(logits, axis=-1)), own)
    weights = jnp.exp(logits - top[:, None])
    own_weight = jnp.exp(own - top)
    total = lax.optimization_barrier(jnp.sum(weights, axis=-1)) + own_weight
    rounded = weights.astype(jnp.bfloat16).astype(jnp.float32)
    summed = jnp.einsum('hl,lhd->hd', rounded, values_f)
    summed = summed + own_weight[:, None] * new_value.reshape(heads, -1).astype(jnp.float32)
    return (summed / total[:, None]).reshape(-1).astype(jnp.bfloat16)

def reference(tokens, gain_attn, w_query, w_key, w_value, w_forget, forget_bias, keys_cache, values_cache, gates_cache, lengths, w_out, gain_mixer, w_up, w_down):
    tokens_f = tokens.astype(jnp.float32)
    attn_scale = lax.rsqrt(lax.optimization_barrier(jnp.mean(tokens_f * tokens_f, axis=-1, keepdims=True)) + norm_eps)
    scaled_in = (tokens_f * gain_attn.astype(jnp.float32)).astype(jnp.bfloat16)
    query = (attn_scale * jnp.dot(scaled_in, w_query, preferred_element_type=jnp.float32)).astype(jnp.bfloat16)
    new_key = (attn_scale * jnp.dot(scaled_in, w_key, preferred_element_type=jnp.float32)).astype(jnp.bfloat16)
    new_value = (attn_scale * jnp.dot(scaled_in, w_value, preferred_element_type=jnp.float32)).astype(jnp.bfloat16)
    forget_log = jax.nn.log_sigmoid(attn_scale * jnp.dot(scaled_in, w_forget, preferred_element_type=jnp.float32) + forget_bias)
    mixed = lax.map(attend_one, (query, keys_cache, values_cache, gates_cache, lengths.astype(jnp.int32), forget_log, new_key, new_value))
    seqs = tokens.shape[0]
    group_width = mixed.shape[1] // N_TP
    mixed_groups = mixed.reshape(seqs, N_TP, group_width).astype(jnp.float32)
    out_groups = w_out.reshape(N_TP, group_width, -1).astype(jnp.float32)
    head_parts = jnp.einsum('bgk,gkd->gbd', mixed_groups, out_groups).astype(jnp.bfloat16)
    head_parts = lax.optimization_barrier(head_parts).astype(jnp.float32)
    residual = (tokens_f + lax.optimization_barrier(jnp.sum(head_parts, axis=0))).astype(jnp.bfloat16)
    residual_f = residual.astype(jnp.float32)
    mixer_scale = lax.rsqrt(lax.optimization_barrier(jnp.mean(residual_f * residual_f, axis=-1, keepdims=True)) + norm_eps)
    scaled_mid = (residual_f * gain_mixer.astype(jnp.float32)).astype(jnp.bfloat16)
    upward = jax.nn.relu(mixer_scale * jnp.dot(scaled_mid, w_up, preferred_element_type=jnp.float32))
    hidden = (upward * upward).astype(jnp.bfloat16)
    down = jnp.dot(hidden, w_down, preferred_element_type=jnp.float32)
    return (residual_f + down).astype(jnp.bfloat16)
```

```python
import functools

import jax
import jax.numpy as jnp
from jax import lax
from jax.experimental import pallas as pl
from jax.experimental.pallas import tpu as pltpu
from jax.sharding import PartitionSpec as P

norm_eps = 1e-06
f32 = jnp.float32
bf16 = jnp.bfloat16
lanes = 128


def padded(width):
    return -(-width // lanes) * lanes


def exchange(pieces, axis):
    return lax.all_to_all(pieces, axis, 0, 0)


def broadcast(piece, axis):
    return exchange(jnp.broadcast_to(piece[None], (lax.axis_size(axis),) + piece.shape), axis)


def split3(value):
    high = value.astype(bf16)
    rest = value - high.astype(f32)
    middle = rest.astype(bf16)
    return high, middle, (rest - middle.astype(f32)).astype(bf16)


def head_mask(heads, width):
    row = lax.broadcasted_iota(jnp.int32, (heads, width), 0)
    column = lax.broadcasted_iota(jnp.int32, (heads, width), 1)
    size = width // heads
    return (column >= row * size) & (column < (row + 1) * size)


def project_kernel(block_ref, gain_ref, wq_ref, wk_ref, wv_ref, wf_ref, out_ref):
    raw = block_ref[...].astype(f32)
    block = (raw * gain_ref[...].astype(f32)).astype(bf16)
    count = out_ref.shape[0]
    gates = jnp.dot(block, wf_ref[...], preferred_element_type=f32)
    squares = jnp.sum(raw * raw, axis=-1, keepdims=True)
    piece = wq_ref.shape[1] // count
    for slot, ref in enumerate((wq_ref, wk_ref, wv_ref)):
        part = jnp.dot(block, ref[...], preferred_element_type=f32)
        for d in range(count):
            out_ref[d, :, slot * piece : (slot + 1) * piece] = part[:, d * piece : (d + 1) * piece]
    heads = gates.shape[1]
    for d in range(count):
        out_ref[d, :, 3 * piece : 3 * piece + heads] = gates
        out_ref[d, :, 3 * piece + heads : 3 * piece + heads + 1] = squares


def attend_kernel(info_ref, qkv_ref, keys_ref, values_ref, gates_ref, out_ref, query_ref):
    seq = pl.program_id(0)
    count = qkv_ref.shape[0]
    piece = qkv_ref.shape[2] // 3
    heads, positions = gates_ref.shape[1], gates_ref.shape[2]
    width = keys_ref.shape[2]
    size = width // heads

    @pl.when(seq == 0)
    def _():
        for d in range(count):
            query_ref[:, d * piece : (d + 1) * piece] = qkv_ref[d, :, :piece].astype(f32)
        out_ref[...] = jnp.zeros(out_ref.shape, f32)

    mask = head_mask(heads, width)
    here = lax.broadcasted_iota(jnp.int32, query_ref.shape, 0) == seq
    query = jnp.sum(jnp.where(here, query_ref[...], 0.0), axis=0, keepdims=True)
    query = jnp.where(mask, query, 0.0).astype(bf16)
    scores = lax.dot_general(
        query, keys_ref[0], (((1,), (1,)), ((), ())), preferred_element_type=f32
    )
    gates = gates_ref[0]
    logits = scores * size ** (-0.5) - gates
    live = info_ref[seq] - info_ref[info_ref.shape[0] - 1] * positions
    where = lax.broadcasted_iota(jnp.int32, (heads, positions), 1)
    valid = where < live
    top = jnp.max(jnp.where(valid, logits, -1e30), axis=-1, keepdims=True)
    weights = jnp.where(valid, jnp.exp(logits - top), 0.0)
    total = jnp.sum(weights, axis=-1, keepdims=True)
    last = jnp.sum(jnp.where(where == live - 1, gates, 0.0), axis=-1, keepdims=True)
    summed = jnp.dot(weights.astype(bf16), values_ref[0], preferred_element_type=f32)
    summed = jnp.sum(jnp.where(mask, summed, 0.0), axis=0, keepdims=True)
    out_ref[:, :width] = jnp.where(here, summed, out_ref[:, :width])
    extra = out_ref.shape[1] - width
    row = lax.broadcasted_iota(jnp.int32, (heads, extra), 0)
    column = lax.broadcasted_iota(jnp.int32, (heads, extra), 1)
    stats = jnp.where(column == row, top, 0.0)
    stats = stats + jnp.where(column == row + heads, total, 0.0)
    stats = stats + jnp.where(column == row + 2 * heads, last, 0.0)
    stats = jnp.sum(stats, axis=0, keepdims=True)
    out_ref[:, width:] = jnp.where(here[:, :extra], stats, out_ref[:, width:])


def combine_kernel(parts_ref, qkv_ref, forget_ref, w_ref, out_ref):
    count = parts_ref.shape[0]
    seqs, heads = forget_ref.shape
    width = w_ref.shape[0]
    piece = qkv_ref.shape[2] // 3
    size = width // heads
    spread = head_mask(heads, width).astype(f32)

    def joined(slot):
        return jnp.concatenate(
            [
                qkv_ref[d, :, slot * piece : (slot + 1) * piece].astype(f32)
                for d in range(count)
            ],
            axis=1,
        )

    query, key, value = joined(0), joined(1), joined(2)
    own = lax.dot_general(
        query * key,
        spread,
        (((1,), (1,)), ((), ())),
        precision=lax.Precision.HIGHEST,
        preferred_element_type=f32,
    ) * size ** (-0.5)
    tops = [parts_ref[d, :, width : width + heads] for d in range(count)]
    peak = functools.reduce(jnp.maximum, tops)
    last = sum(parts_ref[d, :, width + 2 * heads : width + 3 * heads] for d in range(count))
    top = peak + last + forget_ref[...]
    overall = jnp.maximum(top, own)
    shared = jnp.exp(top - overall)
    own_weight = jnp.exp(own - overall)
    factors = [jnp.exp(t - peak) * shared for t in tops]
    total = own_weight
    for d in range(count):
        total = total + parts_ref[d, :, width + heads : width + 2 * heads] * factors[d]
    inverse = 1.0 / total
    small = jnp.concatenate([f * inverse for f in factors] + [own_weight * inverse], axis=0)
    wide = jnp.dot(small, spread, precision=lax.Precision.HIGHEST, preferred_element_type=f32)
    mixed = wide[count * seqs :] * value
    for d in range(count):
        mixed = mixed + wide[d * seqs : (d + 1) * seqs] * parts_ref[d, :, :width]
    out_ref[...] = jnp.dot(
        mixed.astype(bf16), w_ref[...], preferred_element_type=f32
    ).astype(bf16)


def up_kernel(tokens_ref, parts_ref, gain_ref, w_ref, out_ref, residual_ref, scaled_ref, squares_ref):
    @pl.when(pl.program_id(0) == 0)
    def _():
        attended = sum(parts_ref[t].astype(f32) for t in range(parts_ref.shape[0]))
        residual = (tokens_ref[...].astype(f32) + attended).astype(bf16)
        residual_ref[...] = residual
        wide = residual.astype(f32)
        scaled_ref[...] = (wide * gain_ref[...].astype(f32)).astype(bf16)
        squares_ref[...] = jnp.broadcast_to(
            jnp.sum(wide * wide, axis=-1, keepdims=True), squares_ref.shape
        )

    count = out_ref.shape[0]
    piece = w_ref.shape[1] // count
    up = jnp.dot(scaled_ref[...], w_ref[...], preferred_element_type=f32).astype(bf16)
    extra = out_ref.shape[2] - piece
    column = lax.broadcasted_iota(jnp.int32, (up.shape[0], extra), 1)
    squares = squares_ref[:, :1]
    high, middle, low = (part.astype(f32) for part in split3(squares))
    tail = jnp.where(column == 0, high, jnp.where(column == 1, middle, low)).astype(bf16)
    for d in range(count):
        out_ref[d, :, :piece] = up[:, d * piece : (d + 1) * piece]
        out_ref[d, :, piece:] = tail


def down_kernel(hidden_ref, w_ref, out_ref, total_ref):
    step = pl.program_id(0)
    count = hidden_ref.shape[0]
    hidden = jnp.concatenate([hidden_ref[d] for d in range(count)], axis=1)
    down = jnp.dot(hidden, w_ref[...], preferred_element_type=f32)

    @pl.when(step == 0)
    def _():
        total_ref[...] = down

    @pl.when(step > 0)
    def _():
        total_ref[...] += down

    @pl.when(step == pl.num_programs(0) - 1)
    def _():
        groups = out_ref.shape[0]
        part = out_ref.shape[2]
        for t in range(groups):
            out_ref[t] = total_ref[:, t * part : (t + 1) * part]


def shards(
    tokens,
    gain_attn,
    w_query,
    w_key,
    w_value,
    w_forget,
    forget_bias,
    keys_cache,
    values_cache,
    gates_cache,
    lengths,
    w_out,
    gain_mixer,
    w_up,
    w_down,
):
    kv_index = lax.axis_index("kv")
    tp_index = lax.axis_index("tp")
    kv_count = lax.axis_size("kv")
    tp_count = lax.axis_size("tp")
    rows, width = w_query.shape
    seqs, heads, positions = gates_cache.shape
    features = gain_attn.shape[0]
    all_heads = w_forget.shape[1]
    piece = width // kv_count
    row_start = kv_index * rows

    block = lax.all_gather(tokens, "tp", axis=1, tiled=True)
    gain_block = lax.dynamic_slice_in_dim(gain_attn, row_start, rows, 0)[None]
    forget_block = lax.dynamic_slice_in_dim(w_forget, row_start, rows, 0)
    parts = pl.pallas_call(
        project_kernel,
        name="project",
        out_shape=jax.ShapeDtypeStruct((kv_count, seqs, 3 * piece + all_heads + 1), f32),
    )(block, gain_block, w_query, w_key, w_value, forget_block)
    sums = jnp.sum(exchange(parts, "kv"), axis=0)
    scale = lax.rsqrt(sums[:, -1:] / features + norm_eps)
    qkv = broadcast((scale * sums[:, : 3 * piece]).astype(bf16), "kv")
    bias = lax.dynamic_slice_in_dim(forget_bias, tp_index * heads, heads, 0)
    gate_sums = lax.dynamic_slice_in_dim(
        sums[:, 3 * piece : -1], tp_index * heads, heads, 1
    )
    forget_log = jax.nn.log_sigmoid(scale * gate_sums + bias)

    info = jnp.concatenate([lengths, kv_index[None].astype(jnp.int32)])
    wide = width + padded(3 * heads)
    local = pl.pallas_call(
        attend_kernel,
        name="attend",
        grid_spec=pltpu.PrefetchScalarGridSpec(
            num_scalar_prefetch=1,
            grid=(seqs,),
            in_specs=[
                pl.BlockSpec(qkv.shape, lambda b, info: (0, 0, 0)),
                pl.BlockSpec((1, positions, width), lambda b, info: (b, 0, 0)),
                pl.BlockSpec((1, positions, width), lambda b, info: (b, 0, 0)),
                pl.BlockSpec((1, heads, positions), lambda b, info: (b, 0, 0)),
            ],
            out_specs=pl.BlockSpec((seqs, wide), lambda b, info: (0, 0)),
            scratch_shapes=[pltpu.VMEM((seqs, width), f32)],
        ),
        out_shape=jax.ShapeDtypeStruct((seqs, wide), f32),
    )(info, qkv, keys_cache, values_cache, gates_cache)
    gathered = broadcast(local, "kv")
    head_part = pl.pallas_call(
        combine_kernel,
        name="combine",
        out_shape=jax.ShapeDtypeStruct((seqs, w_out.shape[1]), bf16),
    )(gathered, qkv, forget_log, w_out)
    head_parts = lax.all_gather(head_part, "tp")

    hidden_piece = w_up.shape[1] // kv_count
    together = max(1, min(kv_count, 512 // hidden_piece))
    steps = kv_count // together
    up_wide = hidden_piece + padded(hidden_piece + 3) - hidden_piece
    gain_part = lax.dynamic_slice_in_dim(gain_mixer, row_start, rows, 0)[None]
    ups, residual = pl.pallas_call(
        up_kernel,
        name="up",
        grid=(steps,),
        in_specs=[
            pl.BlockSpec(block.shape, lambda s: (0, 0)),
            pl.BlockSpec(head_parts.shape, lambda s: (0, 0, 0)),
            pl.BlockSpec(gain_part.shape, lambda s: (0, 0)),
            pl.BlockSpec((rows, together * hidden_piece), lambda s: (0, s)),
        ],
        out_specs=[
            pl.BlockSpec((together, seqs, up_wide), lambda s: (s, 0, 0)),
            pl.BlockSpec(block.shape, lambda s: (0, 0)),
        ],
        scratch_shapes=[pltpu.VMEM(block.shape, bf16), pltpu.VMEM((seqs, lanes), f32)],
        out_shape=[
            jax.ShapeDtypeStruct((kv_count, seqs, up_wide), bf16),
            jax.ShapeDtypeStruct(block.shape, bf16),
        ],
    )(block, head_parts, gain_part, w_up)
    up_sums = jnp.sum(exchange(ups, "kv").astype(f32), axis=0)
    squares = up_sums[:, hidden_piece : hidden_piece + 3].sum(axis=-1, keepdims=True)
    mixer_scale = lax.rsqrt(squares / features + norm_eps)
    active = jax.nn.relu(mixer_scale * up_sums[:, :hidden_piece])
    hidden = broadcast((active * active).astype(bf16), "kv")
    out_width = w_down.shape[1]
    downs = pl.pallas_call(
        down_kernel,
        name="down",
        grid=(steps,),
        in_specs=[
            pl.BlockSpec((together, seqs, hidden_piece), lambda s: (s, 0, 0)),
            pl.BlockSpec((together * hidden_piece, out_width), lambda s: (s, 0)),
        ],
        out_specs=pl.BlockSpec((tp_count, seqs, out_width // tp_count), lambda s: (0, 0, 0)),
        scratch_shapes=[pltpu.VMEM((seqs, out_width), f32)],
        out_shape=jax.ShapeDtypeStruct((tp_count, seqs, out_width // tp_count), f32),
    )(hidden, w_down)
    mixer = jnp.sum(exchange(downs, "tp"), axis=0)
    mine = lax.dynamic_slice_in_dim(residual, tp_index * mixer.shape[1], mixer.shape[1], 1)
    return (mine.astype(f32) + mixer).astype(bf16)


def solution(mesh):
    return jax.shard_map(
        shards,
        mesh=mesh,
        in_specs=(
            P(None, ("kv", "tp")),
            P(),
            P("kv", "tp"),
            P("kv", "tp"),
            P("kv", "tp"),
            P(),
            P(),
            P(None, "kv", "tp"),
            P(None, "kv", "tp"),
            P(None, "tp", "kv"),
            P(),
            P("tp", "kv"),
            P(),
            P("kv", "tp"),
            P("tp", "kv"),
        ),
        out_specs=P(None, ("kv", "tp")),
        check_vma=False,
    )
```

```python
import functools

import jax
import jax.numpy as jnp
from jax import lax
from jax.experimental import pallas as pl
from jax.experimental.pallas import tpu as pltpu
from jax.sharding import PartitionSpec as P

norm_eps = 1e-06
f32 = jnp.float32
bf16 = jnp.bfloat16
lanes = 128


def padded(width):
    return -(-width // lanes) * lanes


def exchange(pieces, axis):
    return lax.all_to_all(pieces, axis, 0, 0)


def broadcast(piece, axis):
    return exchange(jnp.broadcast_to(piece[None], (lax.axis_size(axis),) + piece.shape), axis)


def split3(value):
    high = value.astype(bf16)
    rest = value - high.astype(f32)
    middle = rest.astype(bf16)
    return high, middle, (rest - middle.astype(f32)).astype(bf16)


def head_mask(heads, width):
    row = lax.broadcasted_iota(jnp.int32, (heads, width), 0)
    column = lax.broadcasted_iota(jnp.int32, (heads, width), 1)
    size = width // heads
    return (column >= row * size) & (column < (row + 1) * size)


def project_kernel(
    info_ref, block_ref, gain_ref, wq_ref, wk_ref, wv_ref, wf_ref, out_ref, key_ref, value_ref
):
    raw = block_ref[...].astype(f32)
    block = (raw * gain_ref[...].astype(f32)).astype(bf16)
    width = wq_ref.shape[1]
    heads = wf_ref.shape[0]
    query = jnp.dot(block, wq_ref[...], preferred_element_type=f32)
    gates = lax.dot_general(
        block, wf_ref[...], (((1,), (1,)), ((), ())), preferred_element_type=f32
    )
    squares = jnp.sum(raw * raw, axis=-1, keepdims=True)
    for d in range(out_ref.shape[0]):
        out_ref[d, :, :width] = query
        out_ref[d, :, width : width + heads] = gates
        out_ref[d, :, width + heads : width + heads + 1] = squares
    key_ref[...] = jnp.dot(block, wk_ref[...], preferred_element_type=f32)
    value_ref[...] = jnp.dot(block, wv_ref[...], preferred_element_type=f32)


def attend_kernel(
    features,
    info_ref,
    parts_ref,
    key_ref,
    value_ref,
    bias_ref,
    keys_ref,
    values_ref,
    gates_ref,
    out_ref,
    forget_ref,
    sums_ref,
    stats_ref,
    keys_near,
    values_near,
    sems,
):
    count = parts_ref.shape[0]
    seqs, heads, positions = gates_ref.shape
    pairs = ((keys_ref, keys_near), (values_ref, values_near))
    copies = [
        [
            pltpu.make_async_copy(source.at[b], target.at[b], sems.at[i, b])
            for i, (source, target) in enumerate(pairs)
        ]
        for b in range(seqs)
    ]
    for both in copies:
        for copy in both:
            copy.start()
    width = keys_ref.shape[2]
    all_heads = bias_ref.shape[1]
    size = width // heads
    step = size ** (-0.5)
    mask = head_mask(heads, width)
    total_in = parts_ref[0]
    for d in range(1, count):
        total_in = total_in + parts_ref[d]
    scale = lax.rsqrt(total_in[:, width + all_heads : width + all_heads + 1] / features + norm_eps)
    query = (scale * total_in[:, :width]).astype(bf16)
    gate = scale * total_in[:, width : width + all_heads] + bias_ref[...]
    log_gate = jnp.minimum(gate, 0.0) - jnp.log1p(jnp.exp(-jnp.abs(gate)))
    row = lax.broadcasted_iota(jnp.int32, (all_heads, heads), 0)
    column = lax.broadcasted_iota(jnp.int32, (all_heads, heads), 1)
    pick = (row == column + info_ref[seqs + 1] * heads).astype(f32)
    forget_ref[...] = jnp.dot(
        log_gate, pick, precision=lax.Precision.HIGHEST, preferred_element_type=f32
    )
    wide = query.astype(f32)
    start = info_ref[seqs] * positions
    where = lax.broadcasted_iota(jnp.int32, (heads, positions), 1)
    lane_row = lax.broadcasted_iota(jnp.int32, (heads, lanes), 0)
    lane = lax.broadcasted_iota(jnp.int32, (heads, lanes), 1)
    for b in range(seqs):
        spread = jnp.where(mask, wide[b : b + 1], 0.0).astype(bf16)
        for copy in copies[b]:
            copy.wait()
        scores = lax.dot_general(
            spread, keys_near[b], (((1,), (1,)), ((), ())), preferred_element_type=f32
        )
        gates = gates_ref[b]
        logits = scores * step - gates
        live = info_ref[b] - start
        valid = where < live
        top = jnp.max(jnp.where(valid, logits, -1e30), axis=-1, keepdims=True)
        weights = jnp.where(valid, jnp.exp(logits - top), 0.0)
        total = jnp.sum(weights, axis=-1, keepdims=True)
        last = jnp.sum(jnp.where(where == live - 1, gates, 0.0), axis=-1, keepdims=True)
        summed = jnp.dot(weights.astype(bf16), values_near[b], preferred_element_type=f32)
        sums_ref[b : b + 1, :] = jnp.sum(jnp.where(mask, summed, 0.0), axis=0, keepdims=True)
        stats = jnp.where(lane == lane_row, top, 0.0)
        stats = jnp.where(lane == lane_row + heads, total, stats)
        stats = jnp.where(lane == lane_row + 2 * heads, last, stats)
        stats_ref[b : b + 1, :] = jnp.sum(stats, axis=0, keepdims=True)
    own = lax.dot_general(
        wide * key_ref[...],
        mask.astype(f32),
        (((1,), (1,)), ((), ())),
        precision=lax.Precision.HIGHEST,
        preferred_element_type=f32,
    ) * (scale * step)
    sums = sums_ref[...].astype(bf16)
    value = (scale * value_ref[...]).astype(bf16)
    tails = split3(stats_ref[:, : 3 * heads]) + split3(own)
    spots = [2 * width + 4 * heads * i for i in range(3)]
    spots = spots + [spot + 3 * heads for spot in spots]
    for d in range(count):
        out_ref[d, :, :width] = sums
        out_ref[d, :, width : 2 * width] = value
        for spot, tail in zip(spots, tails):
            out_ref[d, :, spot : spot + tail.shape[1]] = tail


def combine_kernel(parts_ref, forget_ref, w_ref, out_ref):
    count = parts_ref.shape[0]
    seqs, heads = forget_ref.shape
    width = w_ref.shape[0]
    spread = head_mask(heads, width).astype(f32)
    stats = []
    for d in range(count):
        tails = [
            parts_ref[d, :, 2 * width + 4 * heads * i : 2 * width + 4 * heads * (i + 1)].astype(f32)
            for i in range(3)
        ]
        stats.append(tails[0] + tails[1] + tails[2])
    tops = [part[:, :heads] for part in stats]
    peak = functools.reduce(jnp.maximum, tops)
    joint = functools.reduce(jnp.add, stats)
    own = joint[:, 3 * heads :]
    top = peak + joint[:, 2 * heads : 3 * heads] + forget_ref[...]
    overall = jnp.maximum(top, own)
    shared = jnp.exp(top - overall)
    own_weight = jnp.exp(own - overall)
    factors = [jnp.exp(t - peak) * shared for t in tops]
    total = own_weight
    for d in range(count):
        total = total + stats[d][:, heads : 2 * heads] * factors[d]
    inverse = 1.0 / total
    small = jnp.concatenate([f * inverse for f in factors] + [own_weight * inverse], axis=0)
    wide = jnp.dot(small, spread, precision=lax.Precision.HIGHEST, preferred_element_type=f32)
    value = parts_ref[0, :, width : 2 * width].astype(f32)
    for d in range(1, count):
        value = value + parts_ref[d, :, width : 2 * width].astype(f32)
    mixed = wide[count * seqs :] * value
    for d in range(count):
        mixed = mixed + wide[d * seqs : (d + 1) * seqs] * parts_ref[d, :, :width].astype(f32)
    out_ref[...] = jnp.dot(
        mixed.astype(bf16), w_ref[...], preferred_element_type=f32
    ).astype(bf16)


def started(sources, targets, sems):
    copies = [
        pltpu.make_async_copy(source, target, sems.at[i])
        for i, (source, target) in enumerate(zip(sources, targets))
    ]
    for copy in copies:
        copy.start()
    return copies


def up_kernel(
    together, tokens_ref, parts_ref, gain_ref, w_ref, out_ref, residual_ref, near_ref, sems
):
    count = out_ref.shape[0]
    block = w_ref.shape[1] // near_ref.shape[0]
    piece = w_ref.shape[1] // count
    steps = near_ref.shape[0]
    copies = started(
        [w_ref.at[:, s * block : (s + 1) * block] for s in range(steps)],
        [near_ref.at[s] for s in range(steps)],
        sems,
    )
    attended = sum(parts_ref[t].astype(f32) for t in range(parts_ref.shape[0]))
    residual = (tokens_ref[...].astype(f32) + attended).astype(bf16)
    residual_ref[...] = residual
    wide = residual.astype(f32)
    scaled = (wide * gain_ref[...].astype(f32)).astype(bf16)
    tails = split3(jnp.sum(wide * wide, axis=-1, keepdims=True))
    for s in range(steps):
        copies[s].wait()
        up = jnp.dot(scaled, near_ref[s], preferred_element_type=f32).astype(bf16)
        for d in range(together):
            out_ref[s * together + d, :, :piece] = up[:, d * piece : (d + 1) * piece]
            for i, tail in enumerate(tails):
                out_ref[s * together + d, :, piece + i : piece + i + 1] = tail


def down_kernel(together, hidden_ref, w_ref, out_ref, near_ref, sems):
    steps = near_ref.shape[0]
    block = near_ref.shape[1]
    copies = started(
        [w_ref.at[s * block : (s + 1) * block] for s in range(steps)],
        [near_ref.at[s] for s in range(steps)],
        sems,
    )
    down = 0.0
    for s in range(steps):
        hidden = jnp.concatenate(
            [hidden_ref[s * together + d] for d in range(together)], axis=1
        )
        copies[s].wait()
        down = down + jnp.dot(hidden, near_ref[s], preferred_element_type=f32)
    groups = out_ref.shape[0]
    part = out_ref.shape[2]
    for t in range(groups):
        out_ref[t] = down[:, t * part : (t + 1) * part]


def far(value):
    return pltpu.with_memory_space_constraint(value, pltpu.HBM)


in_vmem = pl.BlockSpec(memory_space=pltpu.VMEM)
in_hbm = pl.BlockSpec(memory_space=pltpu.HBM)
in_smem = pl.BlockSpec(memory_space=pltpu.SMEM)
small_limit = pltpu.CompilerParams(vmem_limit_bytes=16 * 2**20)


def shards(
    tokens,
    gain_attn,
    w_query,
    w_key,
    w_value,
    w_forget,
    forget_bias,
    keys_cache,
    values_cache,
    gates_cache,
    lengths,
    w_out,
    gain_mixer,
    w_up,
    w_down,
):
    kv_index = lax.axis_index("kv")
    tp_index = lax.axis_index("tp")
    kv_count = lax.axis_size("kv")
    tp_count = lax.axis_size("tp")
    rows, width = w_query.shape
    seqs, heads, positions = gates_cache.shape
    features = gain_attn.shape[0]
    all_heads = w_forget.shape[1]
    place = jnp.stack([kv_index, tp_index]).astype(jnp.int32)
    info = jnp.concatenate([lengths, place])

    block = lax.all_gather(tokens, "tp", axis=1, tiled=True)
    whole = pl.BlockSpec((rows, width), lambda s, at: (0, 0))
    small = pl.BlockSpec((seqs, width), lambda s, at: (0, 0))
    part_shape = (kv_count, seqs, width + padded(all_heads + 1))
    parts, part_key, part_value = pl.pallas_call(
        project_kernel,
        name="project",
        grid_spec=pltpu.PrefetchScalarGridSpec(
            num_scalar_prefetch=1,
            grid=(1,),
            in_specs=[
                pl.BlockSpec((seqs, rows), lambda s, at: (0, 0)),
                pl.BlockSpec((1, rows), lambda s, at: (0, at[0])),
                whole,
                whole,
                whole,
                pl.BlockSpec((all_heads, rows), lambda s, at: (0, at[0])),
            ],
            out_specs=[pl.BlockSpec(part_shape, lambda s, at: (0, 0, 0)), small, small],
        ),
        out_shape=[
            jax.ShapeDtypeStruct(part_shape, f32),
            jax.ShapeDtypeStruct((seqs, width), f32),
            jax.ShapeDtypeStruct((seqs, width), f32),
        ],
        compiler_params=small_limit,
    )(place, block, gain_attn[None], far(w_query), far(w_key), far(w_value), far(w_forget.T))

    wide = 2 * width + padded(12 * heads)
    local, forget_log = pl.pallas_call(
        functools.partial(attend_kernel, features),
        name="attend",
        in_specs=[in_smem] + [in_vmem] * 4 + [in_hbm] * 2 + [in_vmem],
        scratch_shapes=[
            pltpu.VMEM((seqs, width), f32),
            pltpu.VMEM((seqs, lanes), f32),
            pltpu.VMEM(keys_cache.shape, bf16),
            pltpu.VMEM(values_cache.shape, bf16),
            pltpu.SemaphoreType.DMA((2, seqs)),
        ],
        out_shape=[
            jax.ShapeDtypeStruct((kv_count, seqs, wide), bf16),
            jax.ShapeDtypeStruct((seqs, heads), f32),
        ],
        compiler_params=pltpu.CompilerParams(vmem_limit_bytes=32 * 2**20),
    )(
        info,
        exchange(parts, "kv"),
        part_key,
        part_value,
        forget_bias[None],
        far(keys_cache),
        far(values_cache),
        gates_cache,
    )
    head_part = pl.pallas_call(
        combine_kernel,
        name="combine",
        in_specs=[in_vmem] * 3,
        out_shape=jax.ShapeDtypeStruct((seqs, w_out.shape[1]), bf16),
        compiler_params=small_limit,
    )(exchange(local, "kv"), forget_log, w_out)
    head_parts = lax.all_gather(head_part, "tp")

    hidden_piece = w_up.shape[1] // kv_count
    together = max(1, min(kv_count, 512 // hidden_piece))
    steps = kv_count // together
    up_wide = padded(hidden_piece + 3)
    gain_part = lax.dynamic_slice_in_dim(gain_mixer, kv_index * rows, rows, 0)[None]
    ups, residual = pl.pallas_call(
        functools.partial(up_kernel, together),
        name="up",
        in_specs=[in_vmem] * 3 + [in_hbm],
        scratch_shapes=[
            pltpu.VMEM((steps, rows, w_up.shape[1] // steps), bf16),
            pltpu.SemaphoreType.DMA((steps,)),
        ],
        out_shape=[
            jax.ShapeDtypeStruct((kv_count, seqs, up_wide), bf16),
            jax.ShapeDtypeStruct(block.shape, bf16),
        ],
        compiler_params=small_limit,
    )(block, head_parts, gain_part, far(w_up))
    up_sums = jnp.sum(exchange(ups, "kv").astype(f32), axis=0)
    squares = up_sums[:, hidden_piece : hidden_piece + 3].sum(axis=-1, keepdims=True)
    mixer_scale = lax.rsqrt(squares / features + norm_eps)
    active = jax.nn.relu(mixer_scale * up_sums[:, :hidden_piece])
    hidden = broadcast((active * active).astype(bf16), "kv")
    out_width = w_down.shape[1]
    downs = pl.pallas_call(
        functools.partial(down_kernel, together),
        name="down",
        in_specs=[in_vmem, in_hbm],
        scratch_shapes=[
            pltpu.VMEM((steps, w_down.shape[0] // steps, out_width), bf16),
            pltpu.SemaphoreType.DMA((steps,)),
        ],
        out_shape=jax.ShapeDtypeStruct((tp_count, seqs, out_width // tp_count), f32),
        compiler_params=small_limit,
    )(hidden, far(w_down))
    mixer = jnp.sum(exchange(downs, "tp"), axis=0)
    mine = lax.dynamic_slice_in_dim(residual, tp_index * mixer.shape[1], mixer.shape[1], 1)
    return (mine.astype(f32) + mixer).astype(bf16)


def solution(mesh):
    return jax.shard_map(
        shards,
        mesh=mesh,
        in_specs=(
            P(None, ("kv", "tp")),
            P(),
            P("kv", "tp"),
            P("kv", "tp"),
            P("kv", "tp"),
            P(),
            P(),
            P(None, "kv", "tp"),
            P(None, "kv", "tp"),
            P(None, "tp", "kv"),
            P(),
            P("tp", "kv"),
            P(),
            P("kv", "tp"),
            P("tp", "kv"),
        ),
        out_specs=P(None, ("kv", "tp")),
        check_vma=False,
    )
```

```python
import functools

import jax
import jax.numpy as jnp
from jax import lax
from jax.experimental import pallas as pl
from jax.experimental.pallas import tpu as pltpu
from jax.sharding import PartitionSpec as P

norm_eps = 1e-06
f32 = jnp.float32
bf16 = jnp.bfloat16
lanes = 128


def padded(width):
    return -(-width // lanes) * lanes


def exchange(pieces, axis):
    return lax.all_to_all(pieces, axis, 0, 0)


def broadcast(piece, axis):
    return exchange(jnp.broadcast_to(piece[None], (lax.axis_size(axis),) + piece.shape), axis)


def split3(value):
    high = value.astype(bf16)
    rest = value - high.astype(f32)
    middle = rest.astype(bf16)
    return high, middle, (rest - middle.astype(f32)).astype(bf16)


def head_mask(heads, width):
    row = lax.broadcasted_iota(jnp.int32, (heads, width), 0)
    column = lax.broadcasted_iota(jnp.int32, (heads, width), 1)
    size = width // heads
    return (column >= row * size) & (column < (row + 1) * size)


def project_kernel(
    info_ref, block_ref, gain_ref, wq_ref, wk_ref, wv_ref, wf_ref, out_ref, key_ref, value_ref
):
    raw = block_ref[...].astype(f32)
    block = (raw * gain_ref[...].astype(f32)).astype(bf16)
    width = wq_ref.shape[1]
    heads = wf_ref.shape[0]
    query = jnp.dot(block, wq_ref[...], preferred_element_type=f32)
    gates = lax.dot_general(
        block, wf_ref[...], (((1,), (1,)), ((), ())), preferred_element_type=f32
    )
    squares = jnp.sum(raw * raw, axis=-1, keepdims=True)
    for d in range(out_ref.shape[0]):
        out_ref[d, :, :width] = query
        out_ref[d, :, width : width + heads] = gates
        out_ref[d, :, width + heads : width + heads + 1] = squares
    key_ref[...] = jnp.dot(block, wk_ref[...], preferred_element_type=f32)
    value_ref[...] = jnp.dot(block, wv_ref[...], preferred_element_type=f32)


def started(sources, targets, sems):
    copies = [
        pltpu.make_async_copy(source, target, sems.at[i])
        for i, (source, target) in enumerate(zip(sources, targets))
    ]
    for copy in copies:
        copy.start()
    return copies


def attend_kernel(
    features,
    info_ref,
    parts_ref,
    key_ref,
    value_ref,
    bias_ref,
    keys_ref,
    values_ref,
    gates_ref,
    out_ref,
    forget_ref,
    sums_ref,
    stats_ref,
    keys_near,
    values_near,
    gates_near,
    bias_near,
    sems,
    side_sems,
):
    count = parts_ref.shape[0]
    seqs, heads, positions = gates_ref.shape
    side = started([bias_ref, gates_ref], [bias_near, gates_near], side_sems)
    pairs = ((keys_ref, keys_near), (values_ref, values_near))
    copies = [
        [
            pltpu.make_async_copy(source.at[b], target.at[b], sems.at[i, b])
            for i, (source, target) in enumerate(pairs)
        ]
        for b in range(seqs)
    ]
    for both in copies:
        for copy in both:
            copy.start()
    width = keys_ref.shape[2]
    all_heads = bias_ref.shape[1]
    size = width // heads
    step = size ** (-0.5)
    mask = head_mask(heads, width)
    total_in = parts_ref[0]
    for d in range(1, count):
        total_in = total_in + parts_ref[d]
    scale = lax.rsqrt(total_in[:, width + all_heads : width + all_heads + 1] / features + norm_eps)
    query = (scale * total_in[:, :width]).astype(bf16)
    side[0].wait()
    gate = scale * total_in[:, width : width + all_heads] + bias_near[...]
    log_gate = jnp.minimum(gate, 0.0) - jnp.log1p(jnp.exp(-jnp.abs(gate)))
    row = lax.broadcasted_iota(jnp.int32, (all_heads, heads), 0)
    column = lax.broadcasted_iota(jnp.int32, (all_heads, heads), 1)
    pick = (row == column + info_ref[seqs + 1] * heads).astype(f32)
    forget_ref[...] = jnp.dot(
        log_gate, pick, precision=lax.Precision.HIGHEST, preferred_element_type=f32
    )
    wide = query.astype(f32)
    side[1].wait()
    start = info_ref[seqs] * positions
    where = lax.broadcasted_iota(jnp.int32, (heads, positions), 1)
    lane_row = lax.broadcasted_iota(jnp.int32, (heads, lanes), 0)
    lane = lax.broadcasted_iota(jnp.int32, (heads, lanes), 1)
    for b in range(seqs):
        spread = jnp.where(mask, wide[b : b + 1], 0.0).astype(bf16)
        for copy in copies[b]:
            copy.wait()
        scores = lax.dot_general(
            spread, keys_near[b], (((1,), (1,)), ((), ())), preferred_element_type=f32
        )
        gates = gates_near[b]
        logits = scores * step - gates
        live = info_ref[b] - start
        valid = where < live
        top = jnp.max(jnp.where(valid, logits, -1e30), axis=-1, keepdims=True)
        weights = jnp.where(valid, jnp.exp(logits - top), 0.0)
        total = jnp.sum(weights, axis=-1, keepdims=True)
        last = jnp.sum(jnp.where(where == live - 1, gates, 0.0), axis=-1, keepdims=True)
        summed = jnp.dot(weights.astype(bf16), values_near[b], preferred_element_type=f32)
        sums_ref[b : b + 1, :] = jnp.sum(jnp.where(mask, summed, 0.0), axis=0, keepdims=True)
        stats = jnp.where(lane == lane_row, top, 0.0)
        stats = jnp.where(lane == lane_row + heads, total, stats)
        stats = jnp.where(lane == lane_row + 2 * heads, last, stats)
        stats_ref[b : b + 1, :] = jnp.sum(stats, axis=0, keepdims=True)
    own = lax.dot_general(
        wide * key_ref[...],
        mask.astype(f32),
        (((1,), (1,)), ((), ())),
        precision=lax.Precision.HIGHEST,
        preferred_element_type=f32,
    ) * (scale * step)
    sums = sums_ref[...].astype(bf16)
    value = (scale * value_ref[...]).astype(bf16)
    tails = split3(stats_ref[:, : 3 * heads]) + split3(own)
    spots = [2 * width + 4 * heads * i for i in range(3)]
    spots = spots + [spot + 3 * heads for spot in spots]
    for d in range(count):
        out_ref[d, :, :width] = sums
        out_ref[d, :, width : 2 * width] = value
        for spot, tail in zip(spots, tails):
            out_ref[d, :, spot : spot + tail.shape[1]] = tail


def combine_kernel(parts_ref, forget_ref, w_ref, out_ref):
    count = parts_ref.shape[0]
    seqs, heads = forget_ref.shape
    width = w_ref.shape[0]
    spread = head_mask(heads, width).astype(f32)
    stats = []
    for d in range(count):
        tails = [
            parts_ref[d, :, 2 * width + 4 * heads * i : 2 * width + 4 * heads * (i + 1)].astype(f32)
            for i in range(3)
        ]
        stats.append(tails[0] + tails[1] + tails[2])
    tops = [part[:, :heads] for part in stats]
    peak = functools.reduce(jnp.maximum, tops)
    joint = functools.reduce(jnp.add, stats)
    own = joint[:, 3 * heads :]
    top = peak + joint[:, 2 * heads : 3 * heads] + forget_ref[...]
    overall = jnp.maximum(top, own)
    shared = jnp.exp(top - overall)
    own_weight = jnp.exp(own - overall)
    factors = [jnp.exp(t - peak) * shared for t in tops]
    total = own_weight
    for d in range(count):
        total = total + stats[d][:, heads : 2 * heads] * factors[d]
    inverse = 1.0 / total
    small = jnp.concatenate([f * inverse for f in factors] + [own_weight * inverse], axis=0)
    wide = jnp.dot(small, spread, precision=lax.Precision.HIGHEST, preferred_element_type=f32)
    value = parts_ref[0, :, width : 2 * width].astype(f32)
    for d in range(1, count):
        value = value + parts_ref[d, :, width : 2 * width].astype(f32)
    mixed = wide[count * seqs :] * value
    for d in range(count):
        mixed = mixed + wide[d * seqs : (d + 1) * seqs] * parts_ref[d, :, :width].astype(f32)
    out_ref[...] = jnp.dot(
        mixed.astype(bf16), w_ref[...], preferred_element_type=f32
    ).astype(bf16)


def up_kernel(
    together, tokens_ref, parts_ref, gain_ref, w_ref, out_ref, residual_ref, near_ref, sems
):
    count = out_ref.shape[0]
    block = w_ref.shape[1] // near_ref.shape[0]
    piece = w_ref.shape[1] // count
    steps = near_ref.shape[0]
    copies = started(
        [w_ref.at[:, s * block : (s + 1) * block] for s in range(steps)],
        [near_ref.at[s] for s in range(steps)],
        sems,
    )
    attended = sum(parts_ref[t].astype(f32) for t in range(parts_ref.shape[0]))
    residual = (tokens_ref[...].astype(f32) + attended).astype(bf16)
    residual_ref[...] = residual
    wide = residual.astype(f32)
    scaled = (wide * gain_ref[...].astype(f32)).astype(bf16)
    tails = split3(jnp.sum(wide * wide, axis=-1, keepdims=True))
    for s in range(steps):
        copies[s].wait()
        up = jnp.dot(scaled, near_ref[s], preferred_element_type=f32).astype(bf16)
        for d in range(together):
            out_ref[s * together + d, :, :piece] = up[:, d * piece : (d + 1) * piece]
            for i, tail in enumerate(tails):
                out_ref[s * together + d, :, piece + i : piece + i + 1] = tail


def down_kernel(together, hidden_ref, w_ref, out_ref, near_ref, sems):
    steps = near_ref.shape[0]
    block = near_ref.shape[1]
    copies = started(
        [w_ref.at[s * block : (s + 1) * block] for s in range(steps)],
        [near_ref.at[s] for s in range(steps)],
        sems,
    )
    down = 0.0
    for s in range(steps):
        hidden = jnp.concatenate(
            [hidden_ref[s * together + d] for d in range(together)], axis=1
        )
        copies[s].wait()
        down = down + jnp.dot(hidden, near_ref[s], preferred_element_type=f32)
    out_ref[...] = down


def far(value):
    return pltpu.with_memory_space_constraint(value, pltpu.HBM)


in_vmem = pl.BlockSpec(memory_space=pltpu.VMEM)
in_hbm = pl.BlockSpec(memory_space=pltpu.HBM)
in_smem = pl.BlockSpec(memory_space=pltpu.SMEM)
small_limit = pltpu.CompilerParams(vmem_limit_bytes=16 * 2**20)


def shards(
    tokens,
    gain_attn,
    w_query,
    w_key,
    w_value,
    w_forget,
    forget_bias,
    keys_cache,
    values_cache,
    gates_cache,
    lengths,
    w_out,
    gain_mixer,
    w_up,
    w_down,
):
    kv_index = lax.axis_index("kv")
    tp_index = lax.axis_index("tp")
    kv_count = lax.axis_size("kv")
    tp_count = lax.axis_size("tp")
    rows, width = w_query.shape
    seqs, heads, positions = gates_cache.shape
    features = gain_attn.shape[0]
    all_heads = w_forget.shape[1]
    place = jnp.stack([kv_index, tp_index]).astype(jnp.int32)
    info = jnp.concatenate([lengths, place])

    block = lax.all_gather(tokens, "tp", axis=1, tiled=True)
    whole = pl.BlockSpec((rows, width), lambda s, at: (0, 0))
    small = pl.BlockSpec((seqs, width), lambda s, at: (0, 0))
    part_shape = (kv_count, seqs, width + padded(all_heads + 1))
    parts, part_key, part_value = pl.pallas_call(
        project_kernel,
        name="project",
        grid_spec=pltpu.PrefetchScalarGridSpec(
            num_scalar_prefetch=1,
            grid=(1,),
            in_specs=[
                pl.BlockSpec((seqs, rows), lambda s, at: (0, 0)),
                pl.BlockSpec((1, rows), lambda s, at: (0, at[0])),
                whole,
                whole,
                whole,
                pl.BlockSpec((all_heads, rows), lambda s, at: (0, at[0])),
            ],
            out_specs=[pl.BlockSpec(part_shape, lambda s, at: (0, 0, 0)), small, small],
        ),
        out_shape=[
            jax.ShapeDtypeStruct(part_shape, f32),
            jax.ShapeDtypeStruct((seqs, width), f32),
            jax.ShapeDtypeStruct((seqs, width), f32),
        ],
        compiler_params=small_limit,
    )(place, block, gain_attn[None], far(w_query), far(w_key), far(w_value), far(w_forget.T))

    wide = 2 * width + padded(12 * heads)
    local, forget_log = pl.pallas_call(
        functools.partial(attend_kernel, features),
        name="attend",
        in_specs=[in_smem] + [in_vmem] * 3 + [in_hbm] * 4,
        scratch_shapes=[
            pltpu.VMEM((seqs, width), f32),
            pltpu.VMEM((seqs, lanes), f32),
            pltpu.VMEM(keys_cache.shape, bf16),
            pltpu.VMEM(values_cache.shape, bf16),
            pltpu.VMEM(gates_cache.shape, f32),
            pltpu.VMEM((1, all_heads), f32),
            pltpu.SemaphoreType.DMA((2, seqs)),
            pltpu.SemaphoreType.DMA((2,)),
        ],
        out_shape=[
            jax.ShapeDtypeStruct((kv_count, seqs, wide), bf16),
            jax.ShapeDtypeStruct((seqs, heads), f32),
        ],
        compiler_params=pltpu.CompilerParams(vmem_limit_bytes=32 * 2**20),
    )(
        info,
        exchange(parts, "kv"),
        part_key,
        part_value,
        far(forget_bias[None]),
        far(keys_cache),
        far(values_cache),
        far(gates_cache),
    )
    head_part = pl.pallas_call(
        combine_kernel,
        name="combine",
        in_specs=[in_vmem] * 3,
        out_shape=jax.ShapeDtypeStruct((seqs, w_out.shape[1]), bf16),
        compiler_params=small_limit,
    )(exchange(local, "kv"), forget_log, w_out)
    head_parts = lax.all_gather(head_part, "tp")

    hidden_piece = w_up.shape[1] // kv_count
    together = max(1, min(kv_count, 512 // hidden_piece))
    steps = kv_count // together
    up_wide = padded(hidden_piece + 3)
    gain_part = lax.dynamic_slice_in_dim(gain_mixer, kv_index * rows, rows, 0)[None]
    ups, residual = pl.pallas_call(
        functools.partial(up_kernel, together),
        name="up",
        in_specs=[in_vmem] * 3 + [in_hbm],
        scratch_shapes=[
            pltpu.VMEM((steps, rows, w_up.shape[1] // steps), bf16),
            pltpu.SemaphoreType.DMA((steps,)),
        ],
        out_shape=[
            jax.ShapeDtypeStruct((kv_count, seqs, up_wide), bf16),
            jax.ShapeDtypeStruct(block.shape, bf16),
        ],
        compiler_params=small_limit,
    )(block, head_parts, gain_part, far(w_up))
    up_sums = jnp.sum(exchange(ups, "kv").astype(f32), axis=0)
    squares = up_sums[:, hidden_piece : hidden_piece + 3].sum(axis=-1, keepdims=True)
    mixer_scale = lax.rsqrt(squares / features + norm_eps)
    active = jax.nn.relu(mixer_scale * up_sums[:, :hidden_piece])
    hidden = broadcast((active * active).astype(bf16), "kv")
    out_width = w_down.shape[1]
    downs = pl.pallas_call(
        functools.partial(down_kernel, together),
        name="down",
        in_specs=[in_vmem, in_hbm],
        scratch_shapes=[
            pltpu.VMEM((steps, w_down.shape[0] // steps, out_width), bf16),
            pltpu.SemaphoreType.DMA((steps,)),
        ],
        out_shape=jax.ShapeDtypeStruct((seqs, out_width), f32),
        compiler_params=small_limit,
    )(hidden, far(w_down))
    gathered = lax.all_gather(downs, "tp")
    share = out_width // tp_count
    mixer = jnp.sum(lax.dynamic_slice_in_dim(gathered, tp_index * share, share, 2), axis=0)
    mine = lax.dynamic_slice_in_dim(residual, tp_index * share, share, 1)
    return (mine.astype(f32) + mixer).astype(bf16)


def solution(mesh):
    return jax.shard_map(
        shards,
        mesh=mesh,
        in_specs=(
            P(None, ("kv", "tp")),
            P(),
            P("kv", "tp"),
            P("kv", "tp"),
            P("kv", "tp"),
            P(),
            P(),
            P(None, "kv", "tp"),
            P(None, "kv", "tp"),
            P(None, "tp", "kv"),
            P(),
            P("tp", "kv"),
            P(),
            P("kv", "tp"),
            P("tp", "kv"),
        ),
        out_specs=P(None, ("kv", "tp")),
        check_vma=False,
    )
```
